32 devices in a mesh: sp: 8 (over z, y), tp: 4 (over x, core).
Axes of the slice: x: 2, y: 2, z: 4, core: 2. Of those that a mesh axis runs over, the one named last changes fastest.
Arguments:
- inputs: bfloat16 [2048, 4096], P('sp', 'tp'), may hold values from -6 to 6
- input_norm_gain: bfloat16 [4096], replicated, may hold values from 0.099609375 to 1.8984375
- pooling_input_weight: bfloat16 [4096, 2048], P('sp', 'tp'), may hold values from -0.09375 to 0.09375
- query_weight: bfloat16 [4096, 2048], P('sp', 'tp'), may hold values from -0.09375 to 0.09375
- key_weight: bfloat16 [4096, 2048], P('sp', 'tp'), may hold values from -0.09375 to 0.09375
- value_weight: bfloat16 [4096, 2048], P('sp', 'tp'), may hold values from -0.09375 to 0.09375
- gate_weight: bfloat16 [4096, 2048], P('sp', 'tp'), may hold values from -0.09375 to 0.09375
- decay_weight: bfloat16 [4096, 16], replicated, may hold values from -0.25 to 0.25
- strength_weight: bfloat16 [4096, 16], replicated, may hold values from -0.09375 to 0.09375
- pooling_group_map: bfloat16 [16, 128, 128], P('tp'), may hold values from -0.5 to 0.5
- pooling_scale: float32 [2048], P('tp'), may hold values from 0.1 to 1.9
- head_log_decay: float32 [16], P('tp')
- decay_logit_bias: float32 [16], P('tp'), may hold values from -1 to 1
- write_logit_bias: float32 [16], P('tp')
- decay_position_factor: float32 [2048, 16], P('sp', 'tp'), may hold values from 0.28 to 3.25
- decay_position_offset: float32 [2048, 16], P('sp', 'tp'), may hold values from -0.7 to 0
- head_norm_gain: float32 [128], replicated, may hold values from 0.1 to 1.9
- pooling_output_weight: bfloat16 [2048, 4096], P('tp', 'sp'), may hold values from -0.125 to 0.125
- delta_output_weight: bfloat16 [2048, 4096], P('tp', 'sp'), may hold values from -0.125 to 0.125
Outputs:
- mixed_out: bfloat16 [2048, 4096], P('sp', 'tp')
The draws below stay inside these ranges and needn't reach their ends.
All inputs are finite; a program needn't handle non-finite values.
Results may differ from the reference program's by a relative error of at most 0.02.
Values may be sent and summed in bfloat16 or wider, within the bound.
A program may use at most 128 MiB of HBM per device.

```python
import jax
import jax.numpy as jnp
from jax import lax

D = 4096
HD = 128
GH = 16
PG = 16
PC = 128
BLK = 64
TOK_DEV = 256
TOKENS = 2048
PW = 2048
GW = 2048
N_TP = 4


def speed_flags(key):
    share = 0.5
    return jax.random.bernoulli(jax.random.fold_in(key, 11), share, (GH,))


def draw_head_log_decay(key, part):
    quick_heads = speed_flags(key)
    mixing = jax.random.uniform(jax.random.fold_in(key, 12), (GH,), jnp.float32)
    quick_rate = jnp.exp(jnp.log(1.0 / 80.0) + mixing * (jnp.log(1.0 / 25.0) - jnp.log(1.0 / 80.0)))
    slow_rate = jnp.exp(jnp.log(0.03) + mixing * (jnp.log(0.15) - jnp.log(0.03))) / TOKENS
    return jnp.log(jnp.where(quick_heads, quick_rate, slow_rate)).astype(jnp.float32)


def draw_write_logit_bias(key, part):
    quick_heads = speed_flags(key)
    jitter = jax.random.uniform(jax.random.fold_in(key, 13), (GH,), jnp.float32, -0.5, 0.5)
    return jnp.where(quick_heads, jitter, jnp.log(0.3 * HD / TOKENS) + jitter).astype(jnp.float32)


def draw_decay_position_factor(key, part):
    device_count = TOKENS // TOK_DEV
    block_level = jnp.exp(jax.random.uniform(jax.random.fold_in(key, 14), (device_count, GH), jnp.float32, jnp.log(0.4), jnp.log(2.5)))
    jitter = jax.random.uniform(jax.random.fold_in(key, 15), (TOKENS, GH), jnp.float32, 0.7, 1.3)
    return (jnp.repeat(block_level, TOK_DEV, axis=0) * jitter).astype(jnp.float32)


def draw_decay_position_offset(key, part):
    places = jax.random.randint(jax.random.fold_in(key, 16), (2, GH), 0, TOKENS)
    losses = jnp.log(jax.random.uniform(jax.random.fold_in(key, 17), (2, GH), jnp.float32, 0.5, 0.8))
    hit_table = jnp.arange(TOKENS)[:, None, None] == places[None]
    return jnp.sum(jnp.where(hit_table, losses[None], 0.0), axis=1).astype(jnp.float32)


def levels(stream_key, dims, split, least, high):
    level = 1.0
    for axis_at, shards_of in split:
        draws = jax.random.uniform(jax.random.fold_in(jax.random.fold_in(stream_key, 6), axis_at), (shards_of,), jnp.float32, least / len(split), high / len(split))
        level = level * jnp.repeat(jnp.exp(draws), dims[axis_at] // shards_of).reshape((-1,) + (1,) * (len(dims) - 1 - axis_at))
    return level


def centred(rng, dims, deviation, most, shards=(), kind=jnp.bfloat16):
    result = deviation * jax.random.normal(rng, dims, jnp.float32)
    if shards:
        result = result * levels(rng, dims, shards, -0.22, 0.18)
    return jnp.clip(result, -most, most).astype(kind)


def setup_inputs(seed: int = 0) -> dict:
    splits = jax.random.split(jax.random.key(seed), 20)
    return {
        "inputs": centred(splits[0], (TOKENS, D), 1.0, 6.0, ((0, 8), (1, 4))),
        "input_norm_gain": jnp.clip(1.0 + 0.18 * jax.random.normal(splits[1], (D,), jnp.float32), 0.099609375, 1.8984375).astype(jnp.bfloat16),
        "pooling_input_weight": centred(splits[2], (D, PW), D ** -0.5, 0.09375, ((0, 8), (1, 4))),
        "query_weight": centred(splits[3], (D, GW), D ** -0.5, 0.09375, ((0, 8), (1, 4))),
        "key_weight": centred(splits[4], (D, GW), D ** -0.5, 0.09375, ((0, 8), (1, 4))),
        "value_weight": centred(splits[5], (D, GW), D ** -0.5, 0.09375, ((0, 8), (1, 4))),
        "gate_weight": centred(splits[6], (D, GW), D ** -0.5, 0.09375, ((0, 8), (1, 4))),
        "decay_weight": centred(splits[7], (D, GH), (D // 9) ** -0.5, 0.25),
        "strength_weight": centred(splits[8], (D, GH), D ** -0.5, 0.09375),
        "pooling_group_map": centred(splits[9], (PG, PC, PC), PC ** -0.5, 0.5, ((0, 4),)),
        "pooling_scale": jnp.clip(1.0 + 0.18 * jax.random.normal(splits[10], (PW,), jnp.float32), 0.1, 1.9),
        "head_log_decay": draw_head_log_decay(jax.random.fold_in(splits[19], 71), 0),
        "decay_logit_bias": jnp.clip(jax.random.uniform(splits[12], (GH,), jnp.float32, -1.0, 1.0) * levels(splits[12], (GH,), ((0, 4),), -0.4, 0.0), -1.0, 1.0),
        "write_logit_bias": draw_write_logit_bias(jax.random.fold_in(splits[19], 71), 0),
        "decay_position_factor": draw_decay_position_factor(jax.random.fold_in(splits[19], 71), 0),
        "decay_position_offset": draw_decay_position_offset(jax.random.fold_in(splits[19], 71), 0),
        "head_norm_gain": jnp.clip(1.0 + 0.18 * jax.random.normal(splits[16], (HD,), jnp.float32), 0.1, 1.9),
        "pooling_output_weight": centred(splits[17], (PW, D), PW ** -0.5, 0.125, ((0, 4), (1, 8))),
        "delta_output_weight": centred(splits[18], (GW, D), GW ** -0.5, 0.125, ((0, 4), (1, 8))),
    }


epsilon = 1e-06
highest = lax.Precision.HIGHEST

def unit_rows(matrix):
    return matrix * lax.rsqrt(lax.optimization_barrier(jnp.sum(matrix * matrix, axis=-1, keepdims=True)) + epsilon)

def pool_windows(first_group, group_count):
    group_ids = first_group + jnp.arange(group_count, dtype=jnp.int32)
    return 2 ** (1 + group_ids % 4)

def pool_branch(padded, windows, positions, pooling_group_map, pooling_scale):
    row_count = padded.shape[0] - 16
    window_sum = jnp.zeros(padded[16:].shape, jnp.float32)
    for lag_index in range(16):
        window_part = padded[16 - lag_index:16 - lag_index + row_count]
        window_sum = window_sum + window_part * (lag_index < windows).astype(jnp.float32)[None, :, None]
    counts = jnp.minimum(positions[:, None] + 1, windows[None, :]).astype(jnp.float32)
    mixed = window_sum / counts[..., None] - padded[16:]
    projected = jnp.einsum('tgc,gcd->tgd', mixed, pooling_group_map.astype(jnp.float32), precision=highest)
    return (projected.reshape(row_count, -1) * pooling_scale).astype(jnp.bfloat16)

def delta_rule_inputs(query_row_block, key_matrix_rows, value_row_block, decay_logits, write_logits, head_log_decay, decay_logit_bias, write_logit_bias, decay_position_factor, decay_position_offset):
    row_count = query_row_block.shape[0]
    head_count = head_log_decay.shape[0]

    def heads_of(matrix):
        return jax.nn.silu(matrix.astype(jnp.float32)).reshape(row_count, head_count, HD)
    query_matrix = unit_rows(heads_of(query_row_block)) * HD ** (-0.5)
    incoming_keys = unit_rows(heads_of(key_matrix_rows))
    value_matrix = heads_of(value_row_block)
    write_strength_rows = jax.nn.sigmoid(write_logits + write_logit_bias)
    decay_log_rows = -jnp.exp(head_log_decay) * jax.nn.softplus(decay_logits + decay_logit_bias) * decay_position_factor + decay_position_offset
    return (query_matrix, incoming_keys, value_matrix, write_strength_rows, decay_log_rows)

def block_terms(query_matrix, incoming_keys, value_matrix, write_strength_rows, decay_log_rows):
    length, head_count, head_depth = query_matrix.shape
    blocks = length // BLK

    def regroup(member):
        return member.reshape(blocks, BLK, head_count, -1).transpose(2, 0, 1, 3)
    query_matrix, incoming_keys, value_matrix = (regroup(query_matrix), regroup(incoming_keys), regroup(value_matrix))
    write_strength_rows = write_strength_rows.reshape(blocks, BLK, head_count).transpose(2, 0, 1)
    running = jnp.cumsum(decay_log_rows.reshape(blocks, BLK, head_count).transpose(2, 0, 1), axis=-1)
    positions = jnp.arange(BLK)
    causal = positions[:, None] >= positions[None, :]
    strict = positions[:, None] > positions[None, :]
    spread = running[..., :, None] - running[..., None, :]
    decay_table = jnp.where(causal, jnp.exp(jnp.where(causal, spread, 0.0)), 0.0)
    weighted = incoming_keys * write_strength_rows[..., None]
    lower_part = jnp.where(strict, jnp.einsum('hnid,hnjd->hnij', weighted, incoming_keys, precision=highest) * decay_table, 0.0)
    system = lower_part + jnp.eye(BLK, dtype=jnp.float32)
    corrected = jax.scipy.linalg.solve_triangular(system, value_matrix * write_strength_rows[..., None], lower=True)
    erased = jax.scipy.linalg.solve_triangular(system, weighted * jnp.exp(running)[..., None], lower=True)
    scores = jnp.einsum('hnid,hnjd->hnij', query_matrix, incoming_keys, precision=highest) * decay_table
    query_decayed = query_matrix * jnp.exp(running)[..., None]
    block_total = running[..., -1]
    key_decayed = incoming_keys * jnp.exp(block_total[..., None] - running)[..., None]
    return (corrected, erased, query_decayed, key_decayed, scores, block_total)

def run_blocks(state_start, terms):

    def advance(state_now, pieces):
        corrected, erased, query_decayed, key_decayed, scores, block_total = pieces
        fresh_values = corrected - jnp.einsum('hcd,hde->hce', erased, state_now, precision=highest)
        output = jnp.einsum('hcd,hde->hce', query_decayed, state_now, precision=highest)
        output = output + jnp.einsum('hij,hje->hie', scores, fresh_values, precision=highest)
        state_now = state_now * jnp.exp(block_total)[:, None, None]
        state_now = state_now + jnp.einsum('hcd,hce->hde', key_decayed, fresh_values, precision=highest)
        return (state_now, output)
    stacked = tuple((jnp.moveaxis(member, 1, 0) for member in terms))
    final_state, outputs = lax.scan(advance, state_start, stacked)
    blocks, head_count, block_rows, head_depth = outputs.shape
    return (final_state, outputs.transpose(0, 2, 1, 3).reshape(blocks * block_rows, head_count, head_depth))

def delta_finish(outputs, gate_rows, head_norm_gain):
    row_count, head_count, head_depth = outputs.shape
    scaled = outputs * lax.rsqrt(lax.optimization_barrier(jnp.mean(outputs * outputs, axis=-1, keepdims=True)) + epsilon) * head_norm_gain
    gated = scaled * jax.nn.silu(gate_rows.astype(jnp.float32).reshape(row_count, head_count, head_depth))
    return gated.reshape(row_count, head_count * head_depth).astype(jnp.bfloat16)

def reference(inputs, input_norm_gain, pooling_input_weight, query_weight, key_weight, value_weight, gate_weight, decay_weight, strength_weight, pooling_group_map, pooling_scale, head_log_decay, decay_logit_bias, write_logit_bias, decay_position_factor, decay_position_offset, head_norm_gain, pooling_output_weight, delta_output_weight):
    floats = inputs.astype(jnp.float32)
    normed = (floats * lax.rsqrt(lax.optimization_barrier(jnp.mean(floats * floats, axis=-1, keepdims=True)) + epsilon) * input_norm_gain.astype(jnp.float32)).astype(jnp.bfloat16)
    pool_rows = jnp.dot(normed.astype(jnp.float32), pooling_input_weight.astype(jnp.float32), preferred_element_type=jnp.float32).astype(jnp.bfloat16)
    query_row_block = jnp.dot(normed.astype(jnp.float32), query_weight.astype(jnp.float32), preferred_element_type=jnp.float32).astype(jnp.bfloat16)
    key_matrix_rows = jnp.dot(normed.astype(jnp.float32), key_weight.astype(jnp.float32), preferred_element_type=jnp.float32).astype(jnp.bfloat16)
    value_row_block = jnp.dot(normed.astype(jnp.float32), value_weight.astype(jnp.float32), preferred_element_type=jnp.float32).astype(jnp.bfloat16)
    gate_rows = jnp.dot(normed.astype(jnp.float32), gate_weight.astype(jnp.float32), preferred_element_type=jnp.float32).astype(jnp.bfloat16)
    decay_logits = jnp.dot(normed.astype(jnp.float32), decay_weight.astype(jnp.float32), preferred_element_type=jnp.float32)
    write_logits = jnp.dot(normed.astype(jnp.float32), strength_weight.astype(jnp.float32), preferred_element_type=jnp.float32)
    total_rows = inputs.shape[0]
    padded = jnp.pad(pool_rows.astype(jnp.float32), ((16, 0), (0, 0))).reshape(total_rows + 16, PG, PC)
    pool_out = pool_branch(padded, pool_windows(0, PG), jnp.arange(total_rows, dtype=jnp.int32), pooling_group_map, pooling_scale)
    query_matrix, incoming_keys, value_matrix, write_strength_rows, decay_log_rows = delta_rule_inputs(query_row_block, key_matrix_rows, value_row_block, decay_logits, write_logits, head_log_decay, decay_logit_bias, write_logit_bias, decay_position_factor, decay_position_offset)
    terms = block_terms(query_matrix, incoming_keys, value_matrix, write_strength_rows, decay_log_rows)
    final_state, outputs = run_blocks(jnp.zeros((GH, HD, HD), jnp.float32), terms)
    delta_out = delta_finish(outputs, gate_rows, head_norm_gain)
    pool_group = PW // N_TP
    delta_group = GW // N_TP
    mixed = jnp.zeros((total_rows, D), jnp.float32)
    for group_index in range(N_TP):
        pool_part = jnp.dot(pool_out[:, group_index * pool_group:(group_index + 1) * pool_group].astype(jnp.float32), pooling_output_weight[group_index * pool_group:(group_index + 1) * pool_group].astype(jnp.float32), preferred_element_type=jnp.float32)
        delta_part = jnp.dot(delta_out[:, group_index * delta_group:(group_index + 1) * delta_group].astype(jnp.float32), delta_output_weight[group_index * delta_group:(group_index + 1) * delta_group].astype(jnp.float32), preferred_element_type=jnp.float32)
        rounded = lax.optimization_barrier((pool_part + delta_part).astype(jnp.bfloat16))
        mixed = mixed + rounded.astype(jnp.float32)
    return mixed.astype(jnp.bfloat16)
```

```python
import jax
import jax.numpy as jnp
from jax import lax
from jax.sharding import PartitionSpec as P

HD = 128
PC = 128
BLK = 64
PAIR = 2


epsilon = 1e-06
highest = lax.Precision.HIGHEST


def shifted(value, axis, steps):
    count = lax.axis_size(axis)
    leading, last = (max(0, -steps), min(count, count - steps))
    return lax.ppermute(value, axis, [(source, source + steps) for source in range(leading, last)])


def unit_rows(matrix):
    return matrix * lax.rsqrt(jnp.sum(matrix * matrix, axis=-1, keepdims=True) + epsilon)


def pool_windows(first_group, group_count):
    group_ids = first_group + jnp.arange(group_count, dtype=jnp.int32)
    return 2 ** (1 + group_ids % 4)


def pool_branch(padded, windows, positions, pooling_group_map, pooling_scale):
    row_count = padded.shape[0] - 16
    window_sum = jnp.zeros(padded[16:].shape, jnp.float32)
    for lag_index in range(16):
        window_part = padded[16 - lag_index : 16 - lag_index + row_count]
        window_sum = (
            window_sum + window_part * (lag_index < windows).astype(jnp.float32)[None, :, None]
        )
    counts = jnp.minimum(positions[:, None] + 1, windows[None, :]).astype(jnp.float32)
    mixed = window_sum / counts[..., None] - padded[16:]
    projected = jnp.einsum(
        "tgc,gcd->tgd", mixed, pooling_group_map.astype(jnp.float32), precision=highest
    )
    return (projected.reshape(row_count, -1) * pooling_scale).astype(jnp.bfloat16)


def delta_rule_inputs(
    query_row_block,
    key_matrix_rows,
    value_row_block,
    decay_logits,
    write_logits,
    head_log_decay,
    decay_logit_bias,
    write_logit_bias,
    decay_position_factor,
    decay_position_offset,
):
    row_count = query_row_block.shape[0]
    head_count = head_log_decay.shape[0]

    def heads_of(matrix):
        return jax.nn.silu(matrix.astype(jnp.float32)).reshape(row_count, head_count, HD)

    query_matrix = unit_rows(heads_of(query_row_block)) * HD ** (-0.5)
    incoming_keys = unit_rows(heads_of(key_matrix_rows))
    value_matrix = heads_of(value_row_block)
    write_strength_rows = jax.nn.sigmoid(write_logits + write_logit_bias)
    decay_log_rows = (
        -jnp.exp(head_log_decay)
        * jax.nn.softplus(decay_logits + decay_logit_bias)
        * decay_position_factor
        + decay_position_offset
    )
    return (query_matrix, incoming_keys, value_matrix, write_strength_rows, decay_log_rows)


def unit_lower_inverse(lower_part):
    size = lower_part.shape[-1]
    rows, columns = jnp.arange(size)[:, None], jnp.arange(size)[None, :]
    identity = jnp.eye(size, dtype=jnp.float32)
    span = 16
    power = jnp.where(rows // span == columns // span, lower_part, 0.0)
    inverse = identity - power
    reach = 2
    while reach < span:
        power = jnp.matmul(power, power, precision=highest)
        inverse = inverse + jnp.matmul(inverse, power, precision=highest)
        reach *= 2
    while span < size:
        across = (rows // span != columns // span) & (
            rows // (2 * span) == columns // (2 * span)
        )
        link = jnp.where(across, lower_part, 0.0)
        inverse = inverse - jnp.matmul(
            jnp.matmul(inverse, link, precision=highest), inverse, precision=highest
        )
        span *= 2
    return inverse


def block_terms(query_matrix, incoming_keys, value_matrix, write_strength_rows, decay_log_rows):
    length, head_count, head_depth = query_matrix.shape
    blocks = length // BLK

    def regroup(member):
        return member.reshape(blocks, BLK, head_count, -1).transpose(2, 0, 1, 3)

    query_matrix, incoming_keys, value_matrix = (
        regroup(query_matrix),
        regroup(incoming_keys),
        regroup(value_matrix),
    )
    write_strength_rows = write_strength_rows.reshape(blocks, BLK, head_count).transpose(2, 0, 1)
    running = jnp.cumsum(
        decay_log_rows.reshape(blocks, BLK, head_count).transpose(2, 0, 1), axis=-1
    )
    positions = jnp.arange(BLK)
    causal = positions[:, None] >= positions[None, :]
    strict = positions[:, None] > positions[None, :]
    spread = running[..., :, None] - running[..., None, :]
    decay_table = jnp.where(causal, jnp.exp(jnp.where(causal, spread, 0.0)), 0.0)
    weighted = incoming_keys * write_strength_rows[..., None]
    lower_part = jnp.where(
        strict,
        jnp.einsum("hnid,hnjd->hnij", weighted, incoming_keys, precision=highest) * decay_table,
        0.0,
    )
    inverse = unit_lower_inverse(lower_part)
    right_sides = jnp.concatenate(
        [value_matrix * write_strength_rows[..., None], weighted * jnp.exp(running)[..., None]],
        axis=-1,
    )
    solved = jnp.matmul(inverse, right_sides, precision=highest)
    corrected, erased = solved[..., :head_depth], solved[..., head_depth:]
    scores = (
        jnp.einsum("hnid,hnjd->hnij", query_matrix, incoming_keys, precision=highest) * decay_table
    )
    query_decayed = query_matrix * jnp.exp(running)[..., None]
    block_total = running[..., -1]
    key_decayed = incoming_keys * jnp.exp(block_total[..., None] - running)[..., None]
    return (corrected, erased, query_decayed, key_decayed, scores, block_total)


def run_blocks(state_start, terms):

    def advance(state_now, pieces):
        corrected, erased, query_decayed, key_decayed, scores, block_total = pieces
        fresh_values = corrected - jnp.einsum("hcd,hde->hce", erased, state_now, precision=highest)
        output = jnp.einsum("hcd,hde->hce", query_decayed, state_now, precision=highest)
        output = output + jnp.einsum("hij,hje->hie", scores, fresh_values, precision=highest)
        state_now = state_now * jnp.exp(block_total)[:, None, None]
        state_now = state_now + jnp.einsum(
            "hcd,hce->hde", key_decayed, fresh_values, precision=highest
        )
        return (state_now, output)

    stacked = tuple((jnp.moveaxis(member, 1, 0) for member in terms))
    final_state, outputs = lax.scan(advance, state_start, stacked)
    blocks, head_count, block_rows, head_depth = outputs.shape
    return (
        final_state,
        outputs.transpose(0, 2, 1, 3).reshape(blocks * block_rows, head_count, head_depth),
    )


def compose_maps(terms):
    corrected, erased, query_decayed, key_decayed, scores, block_total = terms
    head_count, blocks, block_rows, head_depth = corrected.shape
    start_map = jnp.concatenate(
        [
            jnp.broadcast_to(
                jnp.eye(head_depth, dtype=jnp.float32), (head_count, head_depth, head_depth)
            ),
            jnp.zeros((head_count, head_depth, head_depth), jnp.float32),
        ],
        axis=-1,
    )

    def absorb(joined_map, pieces):
        corrected_block, erased_block, key_block, total_block = pieces
        target = jnp.concatenate([jnp.zeros_like(corrected_block), corrected_block], axis=-1)
        residue = target - jnp.einsum("hcd,hde->hce", erased_block, joined_map, precision=highest)
        updated = joined_map * jnp.exp(total_block)[:, None, None]
        updated = updated + jnp.einsum("hcd,hce->hde", key_block, residue, precision=highest)
        return (updated, None)

    stacked = tuple(
        (jnp.moveaxis(member, 1, 0) for member in (corrected, erased, key_decayed, block_total))
    )
    joined_map, unused = lax.scan(absorb, start_map, stacked)
    return (joined_map[..., :head_depth], joined_map[..., head_depth:])


def delta_finish(outputs, gate_rows, head_norm_gain):
    row_count, head_count, head_depth = outputs.shape
    scaled = (
        outputs
        * lax.rsqrt(jnp.mean(outputs * outputs, axis=-1, keepdims=True) + epsilon)
        * head_norm_gain
    )
    gated = scaled * jax.nn.silu(
        gate_rows.astype(jnp.float32).reshape(row_count, head_count, head_depth)
    )
    return gated.reshape(row_count, head_count * head_depth).astype(jnp.bfloat16)


def per_device(
    inputs,
    input_norm_gain,
    pooling_input_weight,
    query_weight,
    key_weight,
    value_weight,
    gate_weight,
    decay_weight,
    strength_weight,
    pooling_group_map,
    pooling_scale,
    head_log_decay,
    decay_logit_bias,
    write_logit_bias,
    decay_position_factor,
    decay_position_offset,
    head_norm_gain,
    pooling_output_weight,
    delta_output_weight,
):
    tok_rows = inputs.shape[0]
    gathered = lax.all_gather(inputs, "tp", axis=1, tiled=True)
    floats = gathered.astype(jnp.float32)
    normed = (
        floats
        * lax.rsqrt(jnp.mean(floats * floats, axis=-1, keepdims=True) + epsilon)
        * input_norm_gain.astype(jnp.float32)
    ).astype(jnp.bfloat16)
    head_count = head_log_decay.shape[0]
    head_first = lax.axis_index("tp") * head_count
    rate_weights = jnp.concatenate(
        [
            lax.dynamic_slice_in_dim(decay_weight, head_first, head_count, 1),
            lax.dynamic_slice_in_dim(strength_weight, head_first, head_count, 1),
        ],
        axis=1,
    )
    rate_rows = jnp.dot(normed, rate_weights, preferred_element_type=jnp.float32)
    decay_logits = rate_rows[:, :head_count]
    write_logits = rate_rows[:, head_count:]
    weights = (pooling_input_weight, query_weight, key_weight, value_weight, gate_weight)
    widths = [member.shape[1] for member in weights]
    joined = jnp.concatenate(weights, axis=1)
    sp_count = lax.axis_size("sp")
    pairs, outer = PAIR, sp_count // PAIR
    me = lax.axis_index("sp")
    mate_weights = lax.ppermute(joined, "sp", [(d, d ^ 1) for d in range(sp_count)])
    is_odd = (me % pairs) == 1
    depth = joined.shape[0]
    my_outer = me // pairs

    def feature_block(which):
        return lax.dynamic_slice_in_dim(normed, which * (pairs * depth), pairs * depth, 1)

    def outer_shift(value, step):
        return lax.ppermute(
            value, "sp", [(d, (d + step * pairs) % sp_count) for d in range(sp_count)]
        )

    arrived = [feature_block(my_outer)]
    for step in range(1, outer):
        arrived.append(outer_shift(feature_block((my_outer + step) % outer), step))
    returned = []
    for step in list(range(1, outer)) + [0]:
        block = arrived[step]
        mine = jnp.where(is_odd, block[:, depth:], block[:, :depth])
        other = jnp.where(is_odd, block[:, :depth], block[:, depth:])
        partial_rows = jnp.dot(mine, joined, preferred_element_type=jnp.float32) + jnp.dot(
            other, mate_weights, preferred_element_type=jnp.float32
        )
        if step:
            returned.append(outer_shift(partial_rows.astype(jnp.bfloat16), outer - step))
        else:
            summed_rows = partial_rows
    for piece in returned:
        summed_rows = summed_rows + piece.astype(jnp.float32)
    split_points = [sum(widths[: split_index + 1]) for split_index in range(len(widths) - 1)]
    projected = jnp.split(summed_rows, split_points, axis=1)
    pool_rows, query_row_block, key_matrix_rows, value_row_block, gate_rows = (
        member.astype(jnp.bfloat16) for member in projected
    )
    previous = shifted(pool_rows[tok_rows - 16 :], "sp", 1)
    group_count = pooling_group_map.shape[0]
    padded = (
        jnp.concatenate([previous, pool_rows], axis=0)
        .astype(jnp.float32)
        .reshape(tok_rows + 16, group_count, PC)
    )
    positions = lax.axis_index("sp") * tok_rows + jnp.arange(tok_rows, dtype=jnp.int32)
    pool_out = pool_branch(
        padded,
        pool_windows(lax.axis_index("tp") * group_count, group_count),
        positions,
        pooling_group_map,
        pooling_scale,
    )
    query_matrix, incoming_keys, value_matrix, write_strength_rows, decay_log_rows = (
        delta_rule_inputs(
            query_row_block,
            key_matrix_rows,
            value_row_block,
            decay_logits,
            write_logits,
            head_log_decay,
            decay_logit_bias,
            write_logit_bias,
            decay_position_factor,
            decay_position_offset,
        )
    )
    terms = block_terms(
        query_matrix, incoming_keys, value_matrix, write_strength_rows, decay_log_rows
    )
    transition = compose_maps(terms)
    packed = jnp.stack(transition).astype(jnp.bfloat16)
    mate_map = lax.ppermute(packed, "sp", [(d, d ^ 1) for d in range(sp_count)]).astype(
        jnp.float32
    )
    first = jnp.where(is_odd, mate_map, jnp.stack(transition))
    second = jnp.where(is_odd, jnp.stack(transition), mate_map)
    joint_move = jnp.matmul(second[0], first[0], precision=highest)
    joint_add = jnp.matmul(second[0], first[1], precision=highest) + second[1]
    state_in = jnp.zeros_like(joint_add)
    for hop in range(outer - 1):
        advanced = joint_add
        if hop:
            advanced = jnp.matmul(joint_move, state_in, precision=highest) + joint_add
        state_in = shifted(advanced.astype(jnp.bfloat16), "sp", pairs).astype(jnp.float32)
    after_first = jnp.matmul(first[0], state_in, precision=highest) + first[1]
    state_in = jnp.where(is_odd, after_first, state_in)
    unused_state, outputs = run_blocks(state_in, terms)
    delta_out = delta_finish(outputs, gate_rows, head_norm_gain)
    both_out = jnp.concatenate([pool_out, delta_out], axis=1)
    out_weights = jnp.concatenate([pooling_output_weight, delta_output_weight], axis=0)
    full_weights = lax.all_gather(out_weights, "sp", axis=1, tiled=True)
    tp_count = lax.axis_size("tp")
    my_tp = lax.axis_index("tp")
    width = full_weights.shape[1] // tp_count
    sent = []
    for step in list(range(1, tp_count)) + [0]:
        columns = lax.dynamic_slice_in_dim(
            full_weights, ((my_tp + step) % tp_count) * width, width, 1
        )
        part = jnp.dot(both_out, columns, preferred_element_type=jnp.float32).astype(jnp.bfloat16)
        if step:
            part = lax.ppermute(
                part, "tp", [(d, (d + step) % tp_count) for d in range(tp_count)]
            )
        sent.append(part)
    summed = sum(part.astype(jnp.float32) for part in sent)
    return summed.astype(jnp.bfloat16)


def solution(mesh):
    placed = (
        P("sp", "tp"),
        P(),
        P("sp", "tp"),
        P("sp", "tp"),
        P("sp", "tp"),
        P("sp", "tp"),
        P("sp", "tp"),
        P(),
        P(),
        P("tp", None, None),
        P("tp"),
        P("tp"),
        P("tp"),
        P("tp"),
        P("sp", "tp"),
        P("sp", "tp"),
        P(),
        P("tp", "sp"),
        P("tp", "sp"),
    )
    return jax.shard_map(
        per_device, mesh=mesh, in_specs=placed, out_specs=P("sp", "tp"), check_vma=False
    )
```

```python
import jax
import jax.numpy as jnp
from jax import lax
from jax.sharding import PartitionSpec as P

HD = 128
PC = 128
BLK = 64
PAIR = 2


epsilon = 1e-06
highest = lax.Precision.HIGH


def shifted(value, axis, steps):
    count = lax.axis_size(axis)
    leading, last = (max(0, -steps), min(count, count - steps))
    return lax.ppermute(value, axis, [(source, source + steps) for source in range(leading, last)])


def unit_rows(matrix):
    return matrix * lax.rsqrt(jnp.sum(matrix * matrix, axis=-1, keepdims=True) + epsilon)


def pool_windows(first_group, group_count):
    group_ids = first_group + jnp.arange(group_count, dtype=jnp.int32)
    return 2 ** (1 + group_ids % 4)


def pool_branch(padded, windows, positions, pooling_group_map, pooling_scale):
    row_count = padded.shape[0] - 16
    window_sum = jnp.zeros(padded[16:].shape, jnp.float32)
    for lag_index in range(16):
        window_part = padded[16 - lag_index : 16 - lag_index + row_count]
        window_sum = (
            window_sum + window_part * (lag_index < windows).astype(jnp.float32)[None, :, None]
        )
    counts = jnp.minimum(positions[:, None] + 1, windows[None, :]).astype(jnp.float32)
    mixed = window_sum / counts[..., None] - padded[16:]
    projected = jnp.einsum(
        "tgc,gcd->tgd", mixed, pooling_group_map.astype(jnp.float32), precision=highest
    )
    return (projected.reshape(row_count, -1) * pooling_scale).astype(jnp.bfloat16)


def delta_rule_inputs(
    query_row_block,
    key_matrix_rows,
    value_row_block,
    decay_logits,
    write_logits,
    head_log_decay,
    decay_logit_bias,
    write_logit_bias,
    decay_position_factor,
    decay_position_offset,
):
    row_count = query_row_block.shape[0]
    head_count = head_log_decay.shape[0]

    def heads_of(matrix):
        return jax.nn.silu(matrix.astype(jnp.float32)).reshape(row_count, head_count, HD)

    query_matrix = unit_rows(heads_of(query_row_block)) * HD ** (-0.5)
    incoming_keys = unit_rows(heads_of(key_matrix_rows))
    value_matrix = heads_of(value_row_block)
    write_strength_rows = jax.nn.sigmoid(write_logits + write_logit_bias)
    decay_log_rows = (
        -jnp.exp(head_log_decay)
        * jax.nn.softplus(decay_logits + decay_logit_bias)
        * decay_position_factor
        + decay_position_offset
    )
    return (query_matrix, incoming_keys, value_matrix, write_strength_rows, decay_log_rows)


def unit_lower_inverse(lower_part):
    size = lower_part.shape[-1]
    rows, columns = jnp.arange(size)[:, None], jnp.arange(size)[None, :]
    identity = jnp.eye(size, dtype=jnp.float32)
    span = 16
    power = jnp.where(rows // span == columns // span, lower_part, 0.0)
    inverse = identity - power
    reach = 2
    while reach < span:
        power = jnp.matmul(power, power, precision=highest)
        inverse = inverse + jnp.matmul(inverse, power, precision=highest)
        reach *= 2
    while span < size:
        across = (rows // span != columns // span) & (
            rows // (2 * span) == columns // (2 * span)
        )
        link = jnp.where(across, lower_part, 0.0)
        inverse = inverse - jnp.matmul(
            jnp.matmul(inverse, link, precision=highest), inverse, precision=highest
        )
        span *= 2
    return inverse


def block_terms(query_matrix, incoming_keys, value_matrix, write_strength_rows, decay_log_rows):
    length, head_count, head_depth = query_matrix.shape
    blocks = length // BLK

    def regroup(member):
        return member.reshape(blocks, BLK, head_count, -1).transpose(2, 0, 1, 3)

    query_matrix, incoming_keys, value_matrix = (
        regroup(query_matrix),
        regroup(incoming_keys),
        regroup(value_matrix),
    )
    write_strength_rows = write_strength_rows.reshape(blocks, BLK, head_count).transpose(2, 0, 1)
    running = jnp.cumsum(
        decay_log_rows.reshape(blocks, BLK, head_count).transpose(2, 0, 1), axis=-1
    )
    positions = jnp.arange(BLK)
    causal = positions[:, None] >= positions[None, :]
    strict = positions[:, None] > positions[None, :]
    spread = running[..., :, None] - running[..., None, :]
    decay_table = jnp.where(causal, jnp.exp(jnp.where(causal, spread, 0.0)), 0.0)
    weighted = incoming_keys * write_strength_rows[..., None]
    lower_part = jnp.where(
        strict,
        jnp.einsum("hnid,hnjd->hnij", weighted, incoming_keys, precision=highest) * decay_table,
        0.0,
    )
    inverse = unit_lower_inverse(lower_part)
    right_sides = jnp.concatenate(
        [value_matrix * write_strength_rows[..., None], weighted * jnp.exp(running)[..., None]],
        axis=-1,
    )
    solved = jnp.matmul(inverse, right_sides, precision=highest)
    corrected, erased = solved[..., :head_depth], solved[..., head_depth:]
    scores = (
        jnp.einsum("hnid,hnjd->hnij", query_matrix, incoming_keys, precision=highest) * decay_table
    )
    query_decayed = query_matrix * jnp.exp(running)[..., None]
    block_total = running[..., -1]
    key_decayed = incoming_keys * jnp.exp(block_total[..., None] - running)[..., None]
    return (corrected, erased, query_decayed, key_decayed, scores, block_total)


def run_blocks(state_start, terms):

    def advance(state_now, pieces):
        corrected, erased, query_decayed, key_decayed, scores, block_total = pieces
        fresh_values = corrected - jnp.einsum("hcd,hde->hce", erased, state_now, precision=highest)
        output = jnp.einsum("hcd,hde->hce", query_decayed, state_now, precision=highest)
        output = output + jnp.einsum("hij,hje->hie", scores, fresh_values, precision=highest)
        state_now = state_now * jnp.exp(block_total)[:, None, None]
        state_now = state_now + jnp.einsum(
            "hcd,hce->hde", key_decayed, fresh_values, precision=highest
        )
        return (state_now, output)

    stacked = tuple((jnp.moveaxis(member, 1, 0) for member in terms))
    final_state, outputs = lax.scan(advance, state_start, stacked, unroll=True)
    blocks, head_count, block_rows, head_depth = outputs.shape
    return (
        final_state,
        outputs.transpose(0, 2, 1, 3).reshape(blocks * block_rows, head_count, head_depth),
    )


def compose_maps(terms):
    corrected, erased, query_decayed, key_decayed, scores, block_total = terms
    head_count, blocks, block_rows, head_depth = corrected.shape
    start_map = jnp.concatenate(
        [
            jnp.broadcast_to(
                jnp.eye(head_depth, dtype=jnp.float32), (head_count, head_depth, head_depth)
            ),
            jnp.zeros((head_count, head_depth, head_depth), jnp.float32),
        ],
        axis=-1,
    )

    def absorb(joined_map, pieces):
        corrected_block, erased_block, key_block, total_block = pieces
        target = jnp.concatenate([jnp.zeros_like(corrected_block), corrected_block], axis=-1)
        residue = target - jnp.einsum("hcd,hde->hce", erased_block, joined_map, precision=highest)
        updated = joined_map * jnp.exp(total_block)[:, None, None]
        updated = updated + jnp.einsum("hcd,hce->hde", key_block, residue, precision=highest)
        return (updated, None)

    stacked = tuple(
        (jnp.moveaxis(member, 1, 0) for member in (corrected, erased, key_decayed, block_total))
    )
    joined_map, unused = lax.scan(absorb, start_map, stacked, unroll=True)
    return (joined_map[..., :head_depth], joined_map[..., head_depth:])


def delta_finish(outputs, gate_rows, head_norm_gain):
    row_count, head_count, head_depth = outputs.shape
    scaled = (
        outputs
        * lax.rsqrt(jnp.mean(outputs * outputs, axis=-1, keepdims=True) + epsilon)
        * head_norm_gain
    )
    gated = scaled * jax.nn.silu(
        gate_rows.astype(jnp.float32).reshape(row_count, head_count, head_depth)
    )
    return gated.reshape(row_count, head_count * head_depth).astype(jnp.bfloat16)


def per_device(
    inputs,
    input_norm_gain,
    pooling_input_weight,
    query_weight,
    key_weight,
    value_weight,
    gate_weight,
    decay_weight,
    strength_weight,
    pooling_group_map,
    pooling_scale,
    head_log_decay,
    decay_logit_bias,
    write_logit_bias,
    decay_position_factor,
    decay_position_offset,
    head_norm_gain,
    pooling_output_weight,
    delta_output_weight,
):
    tok_rows = inputs.shape[0]
    sp_count, tp_count = lax.axis_size("sp"), lax.axis_size("tp")
    pairs, outer = PAIR, sp_count // PAIR
    me, my_tp = lax.axis_index("sp"), lax.axis_index("tp")
    is_odd = (me % pairs) == 1
    my_outer = me // pairs
    joined = jnp.concatenate(
        (pooling_input_weight, query_weight, key_weight, value_weight, gate_weight), axis=1
    )

    def swap(value):
        return lax.ppermute(value, "sp", [(d, d ^ 1) for d in range(sp_count)])

    def outer_shift(value, step):
        return lax.ppermute(
            value, "sp", [(d, (d + step * pairs) % sp_count) for d in range(sp_count)]
        )

    def tp_shift(value, step):
        return lax.ppermute(value, "tp", [(d, (d + step) % tp_count) for d in range(tp_count)])

    feature_width = inputs.shape[1]
    gathered = jnp.zeros((tok_rows, feature_width * tp_count), inputs.dtype)
    for step in range(tp_count):
        piece = tp_shift(inputs, step) if step else inputs
        gathered = lax.dynamic_update_slice_in_dim(
            gathered, piece, ((my_tp - step) % tp_count) * feature_width, 1
        )
    mate_weights = swap(joined)
    out_weights = jnp.concatenate([pooling_output_weight, delta_output_weight], axis=0)
    out_columns = out_weights.shape[1]
    held_weights = {0: out_weights}
    if outer > 1:
        held_weights[1] = outer_shift(out_weights, 1)
    if outer > 2:
        held_weights[outer - 1] = outer_shift(out_weights, outer - 1)
    floats = gathered.astype(jnp.float32)
    normed = (
        floats
        * lax.rsqrt(jnp.mean(floats * floats, axis=-1, keepdims=True) + epsilon)
        * input_norm_gain.astype(jnp.float32)
    ).astype(jnp.bfloat16)
    head_count = head_log_decay.shape[0]
    head_first = lax.axis_index("tp") * head_count
    rate_weights = jnp.concatenate(
        [
            lax.dynamic_slice_in_dim(decay_weight, head_first, head_count, 1),
            lax.dynamic_slice_in_dim(strength_weight, head_first, head_count, 1),
        ],
        axis=1,
    )
    rate_rows = jnp.dot(normed, rate_weights, preferred_element_type=jnp.float32)
    decay_logits = rate_rows[:, :head_count]
    write_logits = rate_rows[:, head_count:]
    weights = (pooling_input_weight, query_weight, key_weight, value_weight, gate_weight)
    widths = [member.shape[1] for member in weights]
    depth = joined.shape[0]

    def feature_block(which):
        return lax.dynamic_slice_in_dim(normed, which * (pairs * depth), pairs * depth, 1)

    half = outer // 2
    arrived = {0: feature_block(my_outer)}
    for step in [half] + [step for step in range(1, outer) if step != half]:
        arrived[step] = outer_shift(feature_block((my_outer + step) % outer), step)

    def partial_for(distance):
        block = arrived[(outer - distance) % outer]
        mine = jnp.where(is_odd, block[:, depth:], block[:, :depth])
        other = jnp.where(is_odd, block[:, :depth], block[:, depth:])
        return jnp.dot(mine, joined, preferred_element_type=jnp.float32) + jnp.dot(
            other, mate_weights, preferred_element_type=jnp.float32
        )

    far = partial_for(half).astype(jnp.bfloat16)
    cut = far.shape[1] // 2
    plus, minus = far[:, :cut], far[:, cut:]
    for distance in range(half - 1, -1, -1):
        got_plus = outer_shift(plus, 1).astype(jnp.float32)
        got_minus = outer_shift(minus, outer - 1).astype(jnp.float32)
        if distance == half - 1:
            got_plus = jnp.pad(got_plus, ((0, 0), (0, far.shape[1] - cut)))
            got_minus = jnp.pad(got_minus, ((0, 0), (cut, 0)))
        if distance:
            plus = (partial_for(distance) + got_plus).astype(jnp.bfloat16)
            minus = (partial_for(outer - distance) + got_minus).astype(jnp.bfloat16)
        else:
            summed_rows = partial_for(0) + got_plus + got_minus
    half_rows = out_weights.shape[0] // 2
    ahead, behind, summed_rows = lax.optimization_barrier(
        (held_weights[1], held_weights[outer - 1], summed_rows)
    )
    for distance in range(2, half + 1):
        if distance < half or outer % 2:
            ahead, behind = outer_shift(ahead, 1), outer_shift(behind, outer - 1)
            held_weights[distance], held_weights[outer - distance] = ahead, behind
        else:
            held_weights[distance] = jnp.concatenate(
                [
                    outer_shift(ahead[:half_rows], 1),
                    outer_shift(behind[half_rows:], outer - 1),
                ],
                axis=0,
            )
    row_weights = jnp.zeros((out_weights.shape[0], outer * out_columns), out_weights.dtype)
    for step in range(outer):
        row_weights = lax.dynamic_update_slice_in_dim(
            row_weights, held_weights[step], ((my_outer - step) % outer) * out_columns, 1
        )
    split_points = [sum(widths[: split_index + 1]) for split_index in range(len(widths) - 1)]
    projected = jnp.split(summed_rows, split_points, axis=1)
    pool_rows, query_row_block, key_matrix_rows, value_row_block, gate_rows = (
        member.astype(jnp.bfloat16) for member in projected
    )
    previous = shifted(pool_rows[tok_rows - 16 :], "sp", 1)
    group_count = pooling_group_map.shape[0]
    padded = (
        jnp.concatenate([previous, pool_rows], axis=0)
        .astype(jnp.float32)
        .reshape(tok_rows + 16, group_count, PC)
    )
    positions = lax.axis_index("sp") * tok_rows + jnp.arange(tok_rows, dtype=jnp.int32)
    pool_out = pool_branch(
        padded,
        pool_windows(lax.axis_index("tp") * group_count, group_count),
        positions,
        pooling_group_map,
        pooling_scale,
    )
    query_matrix, incoming_keys, value_matrix, write_strength_rows, decay_log_rows = (
        delta_rule_inputs(
            query_row_block,
            key_matrix_rows,
            value_row_block,
            decay_logits,
            write_logits,
            head_log_decay,
            decay_logit_bias,
            write_logit_bias,
            decay_position_factor,
            decay_position_offset,
        )
    )
    terms = block_terms(
        query_matrix, incoming_keys, value_matrix, write_strength_rows, decay_log_rows
    )
    transition = compose_maps(terms)
    packed = jnp.stack(transition).astype(jnp.bfloat16)
    mate_map = lax.ppermute(packed, "sp", [(d, d ^ 1) for d in range(sp_count)]).astype(
        jnp.float32
    )
    first = jnp.where(is_odd, mate_map, jnp.stack(transition))
    second = jnp.where(is_odd, jnp.stack(transition), mate_map)
    joint_move = jnp.matmul(second[0], first[0], precision=highest)
    joint_add = jnp.matmul(second[0], first[1], precision=highest) + second[1]
    state_in = jnp.zeros_like(joint_add)
    for hop in range(outer - 1):
        advanced = joint_add
        if hop:
            advanced = jnp.matmul(joint_move, state_in, precision=highest) + joint_add
        state_in = shifted(advanced.astype(jnp.bfloat16), "sp", pairs).astype(jnp.float32)
    after_first = jnp.matmul(first[0], state_in, precision=highest) + first[1]
    state_in = jnp.where(is_odd, after_first, state_in)
    unused_state, outputs = run_blocks(state_in, terms)
    delta_out = delta_finish(outputs, gate_rows, head_norm_gain)
    both_out = jnp.concatenate([pool_out, delta_out], axis=1)
    mate_out = jnp.concatenate([swap(pool_out), swap(delta_out)], axis=1)
    two_out = jnp.concatenate([both_out, mate_out], axis=0)
    width = row_weights.shape[1] // tp_count
    sent = []
    for step in list(range(1, tp_count)) + [0]:
        columns = lax.dynamic_slice_in_dim(
            row_weights, ((my_tp + step) % tp_count) * width, width, 1
        )
        part = jnp.dot(two_out, columns, preferred_element_type=jnp.float32).astype(jnp.bfloat16)
        sent.append(tp_shift(part, step) if step else part)
    summed = sum(part.astype(jnp.float32) for part in sent).astype(jnp.bfloat16)
    kept = summed[:tok_rows].reshape(tok_rows, -1, 1, out_columns)
    crossed = swap(summed[tok_rows:]).reshape(tok_rows, -1, 1, out_columns)
    even = jnp.where(is_odd, crossed, kept)
    odd = jnp.where(is_odd, kept, crossed)
    return jnp.concatenate([even, odd], axis=2).reshape(tok_rows, -1)


def solution(mesh):
    placed = (
        P("sp", "tp"),
        P(),
        P("sp", "tp"),
        P("sp", "tp"),
        P("sp", "tp"),
        P("sp", "tp"),
        P("sp", "tp"),
        P(),
        P(),
        P("tp", None, None),
        P("tp"),
        P("tp"),
        P("tp"),
        P("tp"),
        P("sp", "tp"),
        P("sp", "tp"),
        P(),
        P("tp", "sp"),
        P("tp", "sp"),
    )
    return jax.shard_map(
        per_device, mesh=mesh, in_specs=placed, out_specs=P("sp", "tp"), check_vma=False
    )
```
